32 devices in a mesh: sp: 8 (over z, y), tp: 4 (over x, core).
Axes of the slice: x: 2, y: 2, z: 4, core: 2. Of those that a mesh axis runs over, the one named last changes fastest.
Arguments:
- hidden_in: bfloat16 [6144, 4096], P('sp', 'tp'), may hold values from -16 to 16
- norm_gain: bfloat16 [2, 4096], P(None, 'tp'), may hold values from 0.099609375 to 1.8984375
- value_proj: bfloat16 [2, 4096, 1024], P(None, 'tp', 'sp'), may hold values from -0.09375 to 0.09375
- gate_proj: bfloat16 [2, 4096, 1024], P(None, 'tp', 'sp'), may hold values from -0.09375 to 0.09375
- conv_taps: bfloat16 [2, 31, 1024], P(None, None, 'tp'), may hold values from -1 to 1
- conv_bias: bfloat16 [2, 1024], P(None, 'tp'), may hold values from -3 to 3
- group_gain: bfloat16 [2, 1024], P(None, 'tp'), may hold values from 0.099609375 to 1.8984375
- group_shift: bfloat16 [2, 1024], P(None, 'tp'), may hold values from -3 to 3
- out_proj: bfloat16 [2, 1024, 4096], P(None, 'sp', 'tp'), may hold values from -0.1875 to 0.1875
Outputs:
- hidden_out: bfloat16 [6144, 4096], P('sp', 'tp')
The draws below stay inside these ranges and needn't reach their ends.
All inputs are finite; a program needn't handle non-finite values.
Results may differ from the reference program's by a relative error of at most 0.012.
Values may be sent and summed in bfloat16 or wider, within the bound.
A program may use at most 128 MiB of HBM per device.

```python
import jax
import jax.numpy as jnp
from jax import lax

D = 4096
C = 1024
GROUPS = 4
WIDTH = 31
LAYERS = 2
TOKENS = 6144
N_TP = 4


def draw_hidden_in(key, part):
    first_key, second_key, third_key = jax.random.split(jax.random.fold_in(key, 11), 3)
    phase = jax.random.uniform(first_key, (), jnp.float32)
    columns = jnp.arange(D, dtype=jnp.float32) / D
    column_scale = 0.3 + 1.7 * jnp.mod(columns + phase, 1.0)
    base = jnp.clip(jax.random.normal(second_key, (TOKENS, D), jnp.float32), -6.0, 6.0)
    values = base * column_scale[None, :]
    return values.astype(jnp.bfloat16)


def levels(key, shape, shards, low, high):
    level = 1.0
    for dim, parts in shards:
        steps = jax.random.uniform(jax.random.fold_in(jax.random.fold_in(key, 6), dim), (parts,), jnp.float32, low / len(shards), high / len(shards))
        level = level * jnp.repeat(jnp.exp(steps), shape[dim] // parts).reshape((-1,) + (1,) * (len(shape) - 1 - dim))
    return level


def centred(key, shape, deviation, bound, cuts=(), kind=jnp.bfloat16):
    result = deviation * jax.random.normal(key, shape, jnp.float32)
    if cuts:
        result = result * levels(key, shape, cuts, -0.22, 0.18)
    return jnp.clip(result, -bound, bound).astype(kind)


def setup_inputs(seed: int = 0) -> dict:
    arg_keys = jax.random.split(jax.random.key(seed), 10)
    return {
        "hidden_in": draw_hidden_in(jax.random.fold_in(arg_keys[9], 71), 0),
        "norm_gain": jnp.clip(1.0 + 0.18 * jax.random.normal(arg_keys[1], (LAYERS, D), jnp.float32), 0.099609375, 1.8984375).astype(jnp.bfloat16),
        "value_proj": centred(arg_keys[2], (LAYERS, D, C), D ** -0.5, 0.09375, ((1, 4), (2, 8))),
        "gate_proj": centred(arg_keys[3], (LAYERS, D, C), D ** -0.5, 0.09375, ((1, 4), (2, 8))),
        "conv_taps": centred(arg_keys[4], (LAYERS, WIDTH, C), WIDTH ** -0.5, 1.0, ((2, 4),)),
        "conv_bias": centred(arg_keys[5], (LAYERS, C), 0.5, 3.0, ((1, 4),)),
        "group_gain": jnp.clip(1.0 + 0.18 * jax.random.normal(arg_keys[6], (LAYERS, C), jnp.float32), 0.099609375, 1.8984375).astype(jnp.bfloat16),
        "group_shift": centred(arg_keys[7], (LAYERS, C), 0.5, 3.0, ((1, 4),)),
        "out_proj": centred(arg_keys[8], (LAYERS, C, D), C ** -0.5, 0.1875, ((1, 8), (2, 4))),
    }


row_floor = 1e-06
group_floor = 1e-05

def reference(hidden_in, norm_gain, value_proj, gate_proj, conv_taps, conv_bias, group_gain, group_shift, out_proj):
    residual_rows = hidden_in
    part_width = D // N_TP
    group_size = C // GROUPS
    reach_back = WIDTH - 1
    for level in range(LAYERS):
        wide_rows = residual_rows.astype(jnp.float32)
        scale_rows = lax.rsqrt(lax.optimization_barrier(jnp.mean(wide_rows * wide_rows, axis=1, keepdims=True)) + row_floor)
        normed_rows = (wide_rows * scale_rows * norm_gain[level].astype(jnp.float32)[None, :]).astype(jnp.bfloat16)
        value_sum = jnp.zeros((TOKENS, C), jnp.float32)
        gate_sum = jnp.zeros((TOKENS, C), jnp.float32)
        for block in range(N_TP):
            left_edge = block * part_width
            piece_rows = normed_rows[:, left_edge:left_edge + part_width]
            part_value = jnp.dot(piece_rows, value_proj[level, left_edge:left_edge + part_width], preferred_element_type=jnp.float32).astype(jnp.bfloat16)
            part_gate = jnp.dot(piece_rows, gate_proj[level, left_edge:left_edge + part_width], preferred_element_type=jnp.float32).astype(jnp.bfloat16)
            part_value, part_gate = lax.optimization_barrier((part_value, part_gate))
            value_sum = value_sum + part_value.astype(jnp.float32)
            gate_sum = gate_sum + part_gate.astype(jnp.float32)
        gated = (value_sum * jax.nn.sigmoid(gate_sum)).astype(jnp.bfloat16)
        padded = jnp.pad(gated.astype(jnp.float32), ((reach_back, 0), (0, 0)))
        taps = conv_taps[level].astype(jnp.float32)
        filtered = jnp.zeros((TOKENS, C), jnp.float32) + conv_bias[level].astype(jnp.float32)[None, :]
        for offset in range(WIDTH):
            filtered = filtered + taps[offset][None, :] * padded[offset:offset + TOKENS]
        grouped = filtered.reshape(TOKENS, GROUPS, group_size)
        group_mean = lax.optimization_barrier(jnp.mean(grouped, axis=2, keepdims=True))
        centered = grouped - group_mean
        group_var = lax.optimization_barrier(jnp.mean(centered * centered, axis=2, keepdims=True))
        scaled = (centered * lax.rsqrt(group_var + group_floor)).reshape(TOKENS, C)
        scaled = scaled * group_gain[level].astype(jnp.float32)[None, :] + group_shift[level].astype(jnp.float32)[None, :]
        mixed = jax.nn.silu(scaled).astype(jnp.bfloat16)
        update = jnp.dot(mixed, out_proj[level], preferred_element_type=jnp.float32)
        residual_rows = (wide_rows + update).astype(jnp.bfloat16)
    return residual_rows
```

```python
import jax
import jax.numpy as jnp
from jax import lax
from jax.experimental import pallas as pl
from jax.experimental.pallas import tpu as pltpu
from jax.sharding import PartitionSpec as P

D = 4096
C = 1024
GROUPS = 4
WIDTH = 31


row_floor = 1e-06
group_floor = 1e-05


def passed_along(value, axis, steps):
    count = lax.axis_size(axis)
    initial, last = (max(0, -steps), min(count, count - steps))
    return lax.ppermute(value, axis, [(source, source + steps) for source in range(initial, last)])


def rms_normed(residual_rows, gain_part):
    wide_rows = residual_rows.astype(jnp.float32)
    squares = lax.psum(jnp.sum(wide_rows * wide_rows, axis=1), "tp")
    scale_rows = lax.rsqrt(squares / D + row_floor)
    return (wide_rows * scale_rows[:, None] * gain_part.astype(jnp.float32)[None, :]).astype(
        jnp.bfloat16
    )


def gated_input(normed_rows, w_value, w_gate):
    numbers = (((0,), (1,)), ((), ()))
    value_part = lax.dot_general(w_value, normed_rows, numbers, preferred_element_type=jnp.float32)
    gate_part = lax.dot_general(w_gate, normed_rows, numbers, preferred_element_type=jnp.float32)
    summed = lax.psum_scatter(
        jnp.stack([value_part, gate_part], axis=1).astype(jnp.bfloat16),
        "tp",
        scatter_dimension=0,
        tiled=True,
    ).astype(jnp.float32)
    return (summed[:, 0] * jax.nn.sigmoid(summed[:, 1])).astype(jnp.bfloat16)


def depthwise(extended, taps_part, bias_part, out_len):
    widened = extended.astype(jnp.float32)
    taps = taps_part.astype(jnp.float32)
    filtered = (
        jnp.zeros((extended.shape[0], out_len), jnp.float32)
        + bias_part.astype(jnp.float32)[:, None]
    )
    for offset in range(WIDTH):
        filtered = filtered + taps[offset][:, None] * widened[:, offset : offset + out_len]
    return filtered


def group_normed(filtered, gain_part, shift_part, group_size):
    channels, out_len = filtered.shape
    grouped = filtered.reshape(channels // group_size, group_size, out_len)
    group_mean = jnp.mean(grouped, axis=1, keepdims=True)
    centered = grouped - group_mean
    group_var = jnp.mean(centered * centered, axis=1, keepdims=True)
    scaled = (centered * lax.rsqrt(group_var + group_floor)).reshape(channels, out_len)
    scaled = (
        scaled * gain_part.astype(jnp.float32)[:, None] + shift_part.astype(jnp.float32)[:, None]
    )
    return jax.nn.silu(scaled).astype(jnp.bfloat16)


def project_out(mixed, w_out):
    return lax.dot_general(
        lax.all_gather(mixed, "tp", axis=0, tiled=True),
        w_out,
        (((0,), (0,)), ((), ())),
        preferred_element_type=jnp.float32,
    )


def on_device(
    hidden_in,
    norm_gain,
    value_proj,
    gate_proj,
    conv_taps,
    conv_bias,
    group_gain,
    group_shift,
    out_proj,
):
    tok_rows = hidden_in.shape[0]
    layers = norm_gain.shape[0]
    reach_back = WIDTH - 1
    group_size = C // GROUPS
    all_value, all_gate, all_out = (
        lax.all_gather(value_proj, "sp", axis=2, tiled=True),
        lax.all_gather(gate_proj, "sp", axis=2, tiled=True),
        lax.all_gather(out_proj, "sp", axis=1, tiled=True),
    )
    residual_rows = hidden_in
    for level in range(layers):
        w_value, w_gate, w_out = (all_value[level], all_gate[level], all_out[level])
        normed_rows = rms_normed(residual_rows, norm_gain[level])
        gated = gated_input(normed_rows, w_value, w_gate)
        before = passed_along(gated[:, tok_rows - reach_back :], "sp", 1)
        extended = jnp.concatenate([before, gated], axis=1)
        out_len = extended.shape[1] - reach_back
        filtered = depthwise(extended, conv_taps[level], conv_bias[level], out_len)
        mixed = group_normed(filtered, group_gain[level], group_shift[level], group_size)
        update = project_out(mixed, w_out)
        kept_rows = residual_rows
        residual_rows = (kept_rows.astype(jnp.float32) + update).astype(jnp.bfloat16)
    return residual_rows


MESH = pl.DeviceIdType.MESH
HALO = 32
ROW_TILE = 256
CONV_TILE = 64
VMEM_BYTES = 62 * 1024 * 1024


def fused_kernel(
    n_sp,
    n_tp,
    hidden_ref,
    norm_ref,
    value_ref,
    gate_ref,
    taps_ref,
    bias_ref,
    ggain_ref,
    gshift_ref,
    out_proj_ref,
    out_ref,
    w_in,
    w_out,
    scaled,
    part,
    from_core,
    to_chip,
    from_chip,
    extended,
    halo_send,
    halo_recv,
    mixed,
    squares,
    load_sem,
    w_send,
    w_recv,
    t_send,
    t_recv,
    s_send,
    s_recv,
):
    layers, width = taps_ref.shape[0], taps_ref.shape[1]
    rows, feats = hidden_ref.shape
    piece = value_ref.shape[2]
    blocks = n_sp // n_tp
    channels = blocks * piece
    reach = width - 1
    nz = n_sp // 2
    s = lax.axis_index("sp")
    t = lax.axis_index("tp")
    z, y = s // 2, s % 2
    chip, core = t // 2, t % 2
    core_mate = chip * 2 + (1 - core)
    chip_mate = (1 - chip) * 2 + core
    far_mate = (1 - chip) * 2 + (1 - core)

    loads = []
    for level in range(layers):
        for kind, (source, target) in enumerate(
            (
                (value_ref.at[level], w_in.at[level, s, :, pl.ds(0, piece)]),
                (gate_ref.at[level], w_in.at[level, s, :, pl.ds(piece, piece)]),
                (
                    out_proj_ref.at[level],
                    w_out.at[level, pl.ds(pl.multiple_of(s * piece, piece), piece), :],
                ),
            )
        ):
            copy = pltpu.make_async_copy(source, target, load_sem.at[level, kind])
            copy.start()
            loads.append(copy)

    barrier = pltpu.get_barrier_semaphore()

    def greet(sp_index, tp_index):
        pl.semaphore_signal(barrier, inc=1, device_id=(sp_index, tp_index), device_id_type=MESH)

    up, down = z < nz - 1, z > 0
    corner_up = jnp.logical_and(up, y == 1)
    corner_down = jnp.logical_and(down, y == 0)
    for mate in (core_mate, chip_mate, far_mate):
        greet(s, mate)
    greet(z * 2 + 1 - y, t)
    for condition, target in (
        (up, s + 2),
        (down, s - 2),
        (corner_up, s + 1),
        (corner_down, s - 1),
    ):

        @pl.when(condition)
        def _(target=target):
            greet(target, t)

    mates = 4
    for condition in (up, down, corner_up, corner_down):
        mates = mates + condition.astype(jnp.int32)
    pl.semaphore_wait(barrier, mates)

    for copy in loads:
        copy.wait()

    half = feats // 2
    phases = []
    for level in range(layers):
        phases += [("in", level, 0), ("in", level, 1), ("out", level, 0)]

    def chunk(phase, owner):
        kind, level, part_index = phases[phase]
        if kind == "in":
            return w_in.at[level, owner, pl.ds(part_index * half, half), :]
        return w_out.at[level, pl.ds(pl.multiple_of(owner * piece, piece), piece), :]

    def weight_copy(phase, owner, way):
        target = (s + 2, s - 2, z * 2 + 1 - y)[way]
        return pltpu.make_async_remote_copy(
            src_ref=chunk(phase, owner),
            dst_ref=chunk(phase, owner),
            send_sem=w_send.at[phase, way, owner],
            recv_sem=w_recv.at[phase, owner],
            device_id=(target, t),
            device_id_type=MESH,
        )

    def own(phase):
        @pl.when(up)
        def _():
            weight_copy(phase, s, 0).start()

        @pl.when(down)
        def _():
            weight_copy(phase, s, 1).start()

        weight_copy(phase, s, 2).start()

    def hops(phase):
        for hop in range(1, nz):

            @pl.when(z >= hop)
            def _(hop=hop):
                owner = s - 2 * hop
                weight_copy(phase, owner, 0).wait_recv()

                @pl.when(up)
                def _():
                    weight_copy(phase, owner, 0).start()

                weight_copy(phase, owner, 2).start()

            @pl.when(z + hop < nz)
            def _(hop=hop):
                owner = s + 2 * hop
                weight_copy(phase, owner, 1).wait_recv()

                @pl.when(down)
                def _():
                    weight_copy(phase, owner, 1).start()

                weight_copy(phase, owner, 2).start()

    def crossed(phase):
        for z_from in range(nz):
            weight_copy(phase, z_from * 2 + 1 - y, 2).wait_recv()

    def sent(phase):
        for z_from in range(nz):
            owner = z_from * 2 + y

            @pl.when(jnp.logical_and(z >= z_from, up))
            def _(owner=owner):
                weight_copy(phase, owner, 0).wait_send()

            @pl.when(jnp.logical_and(z <= z_from, down))
            def _(owner=owner):
                weight_copy(phase, owner, 1).wait_send()

            weight_copy(phase, owner, 2).wait_send()

    def tp_copy(level, slot, source, target, mate, sp_index=None):
        return pltpu.make_async_remote_copy(
            src_ref=source,
            dst_ref=target,
            send_sem=t_send.at[level, slot],
            recv_sem=t_recv.at[level, slot],
            device_id=(s if sp_index is None else sp_index, mate),
            device_id_type=MESH,
        )

    def prepare(level):
        gain = norm_ref[pl.ds(level, 1), :].astype(jnp.float32)
        ones = jnp.ones((8, feats), jnp.bfloat16)
        numbers = (((1,), (1,)), ((), ()))
        source = hidden_ref if level == 0 else out_ref
        for tile in range(rows // ROW_TILE):
            span = pl.ds(tile * ROW_TILE, ROW_TILE)
            wide = source[span, :].astype(jnp.float32)
            scaled[span, :] = (wide * gain).astype(jnp.bfloat16)
            square = wide * wide
            high = square.astype(jnp.bfloat16)
            low = (square - high.astype(jnp.float32)).astype(jnp.bfloat16)
            total = lax.dot_general(ones, high, numbers, preferred_element_type=jnp.float32)
            total = total + lax.dot_general(ones, low, numbers, preferred_element_type=jnp.float32)
            squares[level, t, :, span] = total
        for slot, mate in enumerate((core_mate, chip_mate, far_mate)):
            square_copy(level, slot, mate).start()

    def square_copy(level, slot, mate):
        return pltpu.make_async_remote_copy(
            src_ref=squares.at[level, t],
            dst_ref=squares.at[level, t],
            send_sem=s_send.at[level, slot],
            recv_sem=s_recv.at[level, slot],
            device_id=(s, mate),
            device_id_type=MESH,
        )

    def row_scales(level):
        for slot, mate in enumerate((core_mate, chip_mate, far_mate)):
            copy = square_copy(level, slot, mate)
            copy.wait_send()
            copy.wait_recv()
        total = squares[level, 0]
        for index in range(1, n_tp):
            total = total + squares[level, index]
        scale = lax.rsqrt(total / D + row_floor)
        return scale.T[:, 0:1]

    def products(level, owner):
        @pl.loop(0, blocks * (rows // ROW_TILE))
        def _(step):
            block = step // (rows // ROW_TILE)
            tile = step % (rows // ROW_TILE)
            span = pl.ds(pl.multiple_of(tile * ROW_TILE, ROW_TILE), ROW_TILE)
            part[owner, block, span, :] = jnp.dot(
                scaled[span, :],
                w_in[level, owner * blocks + block],
                preferred_element_type=jnp.float32,
            ).astype(jnp.bfloat16)

    base = 2 + blocks

    def core_copy(level, slot):
        owner = (far_mate, core_mate)[slot]
        return tp_copy(level, slot, part.at[owner], from_core.at[level, slot], core_mate)

    def chip_copy(level, block):
        return tp_copy(
            level, 2 + block, to_chip.at[block], from_chip.at[level, block], chip_mate
        )

    def halo_copy(level):
        return tp_copy(level, base + 3, halo_send, halo_recv.at[level], t, s + 1)

    def mixed_copy(level, slot):
        owner = (t, t, chip_mate)[slot]
        mate = (core_mate, chip_mate, core_mate)[slot]
        return tp_copy(
            level, base + slot, mixed.at[level, owner], mixed.at[level, owner], mate
        )

    def first_half(level):
        products(level, far_mate)
        core_copy(level, 0).start()
        products(level, chip_mate)
        core_copy(level, 0).wait_recv()
        for block in range(blocks):
            to_chip[block] = (
                part[chip_mate, block].astype(jnp.float32)
                + from_core[level, 0, block].astype(jnp.float32)
            ).astype(jnp.bfloat16)
            chip_copy(level, block).start()
        products(level, core_mate)
        core_copy(level, 1).start()
        products(level, t)
        core_copy(level, 1).wait_recv()

    def gating(level):
        scale = row_scales(level)
        for block in range(blocks):
            lanes = pl.ds(block * piece, piece)
            chip_copy(level, block).wait_recv()
            total = (
                part[t, block].astype(jnp.float32)
                + from_core[level, 1, block].astype(jnp.float32)
                + from_chip[level, block].astype(jnp.float32)
            ) * scale
            gated = (total[:, :piece] * jax.nn.sigmoid(total[:, piece:])).astype(jnp.bfloat16)
            halo_send[:, lanes] = gated[rows - HALO :]
            extended[pl.ds(HALO, rows), lanes] = gated.astype(jnp.float32)

        @pl.when(s < n_sp - 1)
        def _():
            halo_copy(level).start()

    def filtering(level):
        taps = taps_ref[level].astype(jnp.float32)
        bias = bias_ref[pl.ds(level, 1), :].astype(jnp.float32)
        ggain = ggain_ref[pl.ds(level, 1), :].astype(jnp.float32)
        gshift = gshift_ref[pl.ds(level, 1), :].astype(jnp.float32)

        @pl.when(s > 0)
        def _():
            halo_copy(level).wait_recv()
            extended[pl.ds(0, HALO), :] = halo_recv[level].astype(jnp.float32)

        @pl.when(s == 0)
        def _():
            extended[pl.ds(0, HALO), :] = jnp.zeros((HALO, channels), jnp.float32)

        @pl.loop(0, rows // CONV_TILE)
        def _(tile):
            start = pl.multiple_of(tile * CONV_TILE, CONV_TILE)
            window = extended[pl.ds(start, CONV_TILE + HALO), :]
            filtered = jnp.zeros((CONV_TILE, channels), jnp.float32) + bias
            for offset in range(width):
                low = HALO - reach + offset
                filtered = filtered + taps[offset : offset + 1, :] * window[low : low + CONV_TILE]
            mean = jnp.mean(filtered, axis=1, keepdims=True)
            centered = filtered - mean
            var = jnp.mean(centered * centered, axis=1, keepdims=True)
            normed = centered * lax.rsqrt(var + group_floor) * ggain + gshift
            mixed[level, t, pl.ds(start, CONV_TILE), :] = (
                normed * jax.nn.sigmoid(normed)
            ).astype(jnp.bfloat16)

        mixed_copy(level, 1).start()
        mixed_copy(level, 0).start()

    def relay(level):
        mixed_copy(level, 1).wait_recv()
        mixed_copy(level, 2).start()

    def projecting(level):
        mixed_copy(level, 0).wait_recv()
        mixed_copy(level, 2).wait_recv()
        source = hidden_ref if level == 0 else out_ref
        tiles = rows // ROW_TILE

        @pl.loop(0, tiles)
        def _(tile):
            span = pl.ds(pl.multiple_of(tile * ROW_TILE, ROW_TILE), ROW_TILE)
            total = source[span, :].astype(jnp.float32)
            for owner in range(n_tp):
                total = total + jnp.dot(
                    mixed[level, owner, span, :],
                    w_out[level, pl.ds(owner * channels, channels), :],
                    preferred_element_type=jnp.float32,
                )
            out_ref[span, :] = total.astype(jnp.bfloat16)

    def settle(level):
        for slot in range(2):
            core_copy(level, slot).wait_send()
        for block in range(blocks):
            chip_copy(level, block).wait_send()
        for slot in range(3):
            mixed_copy(level, slot).wait_send()

        @pl.when(s < n_sp - 1)
        def _():
            halo_copy(level).wait_send()

    own(0)
    own(1)
    prepare(0)
    for level in range(layers):
        first = 3 * level
        last = level == layers - 1
        if level == 0:
            hops(0)
            own(2)
            hops(1)
            if not last:
                own(3)
        crossed(first)
        crossed(first + 1)
        first_half(level)
        hops(first + 2)
        if not last:
            own(first + 4)
        gating(level)
        filtering(level)
        if not last:
            hops(first + 3)
            own(first + 5)
        relay(level)
        crossed(first + 2)
        projecting(level)
        settle(level)
        if not last:
            prepare(level + 1)
            hops(first + 4)
    for phase in range(len(phases)):
        sent(phase)


def fused(n_sp, n_tp, *arrays):
    hidden_in, norm_gain, value_proj = arrays[:3]
    rows, feats = hidden_in.shape
    layers = norm_gain.shape[0]
    piece = value_proj.shape[2]
    blocks = n_sp // n_tp
    channels = blocks * piece
    kinds = 3
    vmem = pl.BlockSpec(memory_space=pltpu.VMEM)
    hbm = pl.BlockSpec(memory_space=pl.ANY)
    low, wide = jnp.bfloat16, jnp.float32
    slots = 2 + blocks + 4
    return pl.pallas_call(
        lambda *refs: fused_kernel(n_sp, n_tp, *refs),
        out_shape=jax.ShapeDtypeStruct((rows, feats), low),
        in_specs=[vmem, vmem, hbm, hbm, vmem, vmem, vmem, vmem, hbm],
        out_specs=vmem,
        scratch_shapes=[
            pltpu.VMEM((layers, n_sp, feats, 2 * piece), low),
            pltpu.VMEM((layers, n_sp * piece, feats), low),
            pltpu.VMEM((rows, feats), low),
            pltpu.VMEM((n_tp, blocks, rows, 2 * piece), low),
            pltpu.VMEM((layers, 2, blocks, rows, 2 * piece), low),
            pltpu.VMEM((blocks, rows, 2 * piece), low),
            pltpu.VMEM((layers, blocks, rows, 2 * piece), low),
            pltpu.VMEM((HALO + rows, channels), wide),
            pltpu.VMEM((HALO, channels), low),
            pltpu.VMEM((layers, HALO, channels), low),
            pltpu.VMEM((layers, n_tp, rows, channels), low),
            pltpu.VMEM((layers, n_tp, 8, rows), wide),
            pltpu.SemaphoreType.DMA((layers, kinds)),
            pltpu.SemaphoreType.DMA((layers * kinds, 3, n_sp)),
            pltpu.SemaphoreType.DMA((layers * kinds, n_sp)),
            pltpu.SemaphoreType.DMA((layers, slots)),
            pltpu.SemaphoreType.DMA((layers, slots)),
            pltpu.SemaphoreType.DMA((layers, 3)),
            pltpu.SemaphoreType.DMA((layers, 3)),
        ],
        compiler_params=pltpu.CompilerParams(
            collective_id=0, has_side_effects=True, vmem_limit_bytes=VMEM_BYTES
        ),
    )(*arrays)


def solution(mesh):
    n_sp, n_tp = mesh.shape["sp"], mesh.shape["tp"]
    piece = C // n_sp
    small = n_tp == 4 and GROUPS == n_tp and n_sp % n_tp == 0 and piece % 128 == 0

    def local(*arrays):
        if small and arrays[0].shape[0] % ROW_TILE == 0:
            return fused(n_sp, n_tp, *arrays)
        return on_device(*arrays)

    return jax.shard_map(
        local,
        mesh=mesh,
        in_specs=(
            P("sp", "tp"),
            P(None, "tp"),
            P(None, "tp", "sp"),
            P(None, "tp", "sp"),
            P(None, None, "tp"),
            P(None, "tp"),
            P(None, "tp"),
            P(None, "tp"),
            P(None, "sp", "tp"),
        ),
        out_specs=P("sp", "tp"),
        check_vma=False,
    )
```

```python
import jax
import jax.numpy as jnp
from jax import lax
from jax.experimental import pallas as pl
from jax.experimental.pallas import tpu as pltpu
from jax.sharding import PartitionSpec as P

D = 4096
C = 1024
GROUPS = 4
WIDTH = 31


row_floor = 1e-06
group_floor = 1e-05


def passed_along(value, axis, steps):
    count = lax.axis_size(axis)
    initial, last = (max(0, -steps), min(count, count - steps))
    return lax.ppermute(value, axis, [(source, source + steps) for source in range(initial, last)])


def rms_normed(residual_rows, gain_part):
    wide_rows = residual_rows.astype(jnp.float32)
    squares = lax.psum(jnp.sum(wide_rows * wide_rows, axis=1), "tp")
    scale_rows = lax.rsqrt(squares / D + row_floor)
    return (wide_rows * scale_rows[:, None] * gain_part.astype(jnp.float32)[None, :]).astype(
        jnp.bfloat16
    )


def gated_input(normed_rows, w_value, w_gate):
    numbers = (((0,), (1,)), ((), ()))
    value_part = lax.dot_general(w_value, normed_rows, numbers, preferred_element_type=jnp.float32)
    gate_part = lax.dot_general(w_gate, normed_rows, numbers, preferred_element_type=jnp.float32)
    summed = lax.psum_scatter(
        jnp.stack([value_part, gate_part], axis=1).astype(jnp.bfloat16),
        "tp",
        scatter_dimension=0,
        tiled=True,
    ).astype(jnp.float32)
    return (summed[:, 0] * jax.nn.sigmoid(summed[:, 1])).astype(jnp.bfloat16)


def depthwise(extended, taps_part, bias_part, out_len):
    widened = extended.astype(jnp.float32)
    taps = taps_part.astype(jnp.float32)
    filtered = (
        jnp.zeros((extended.shape[0], out_len), jnp.float32)
        + bias_part.astype(jnp.float32)[:, None]
    )
    for offset in range(WIDTH):
        filtered = filtered + taps[offset][:, None] * widened[:, offset : offset + out_len]
    return filtered


def group_normed(filtered, gain_part, shift_part, group_size):
    channels, out_len = filtered.shape
    grouped = filtered.reshape(channels // group_size, group_size, out_len)
    group_mean = jnp.mean(grouped, axis=1, keepdims=True)
    centered = grouped - group_mean
    group_var = jnp.mean(centered * centered, axis=1, keepdims=True)
    scaled = (centered * lax.rsqrt(group_var + group_floor)).reshape(channels, out_len)
    scaled = (
        scaled * gain_part.astype(jnp.float32)[:, None] + shift_part.astype(jnp.float32)[:, None]
    )
    return jax.nn.silu(scaled).astype(jnp.bfloat16)


def project_out(mixed, w_out):
    return lax.dot_general(
        lax.all_gather(mixed, "tp", axis=0, tiled=True),
        w_out,
        (((0,), (0,)), ((), ())),
        preferred_element_type=jnp.float32,
    )


def on_device(
    hidden_in,
    norm_gain,
    value_proj,
    gate_proj,
    conv_taps,
    conv_bias,
    group_gain,
    group_shift,
    out_proj,
):
    tok_rows = hidden_in.shape[0]
    layers = norm_gain.shape[0]
    reach_back = WIDTH - 1
    group_size = C // GROUPS
    all_value, all_gate, all_out = (
        lax.all_gather(value_proj, "sp", axis=2, tiled=True),
        lax.all_gather(gate_proj, "sp", axis=2, tiled=True),
        lax.all_gather(out_proj, "sp", axis=1, tiled=True),
    )
    residual_rows = hidden_in
    for level in range(layers):
        w_value, w_gate, w_out = (all_value[level], all_gate[level], all_out[level])
        normed_rows = rms_normed(residual_rows, norm_gain[level])
        gated = gated_input(normed_rows, w_value, w_gate)
        before = passed_along(gated[:, tok_rows - reach_back :], "sp", 1)
        extended = jnp.concatenate([before, gated], axis=1)
        out_len = extended.shape[1] - reach_back
        filtered = depthwise(extended, conv_taps[level], conv_bias[level], out_len)
        mixed = group_normed(filtered, group_gain[level], group_shift[level], group_size)
        update = project_out(mixed, w_out)
        kept_rows = residual_rows
        residual_rows = (kept_rows.astype(jnp.float32) + update).astype(jnp.bfloat16)
    return residual_rows


MESH = pl.DeviceIdType.MESH
HALO = 32
ROW_TILE = 256
CONV_TILE = 64
VMEM_BYTES = 62 * 1024 * 1024
SPLIT = 3


def fused_kernel(
    n_sp,
    n_tp,
    hidden_ref,
    norm_ref,
    value_ref,
    gate_ref,
    taps_ref,
    bias_ref,
    ggain_ref,
    gshift_ref,
    out_proj_ref,
    out_ref,
    w_in,
    w_out,
    scaled,
    part,
    from_core,
    to_chip,
    from_chip,
    extended,
    halo_send,
    halo_recv,
    mixed,
    squares,
    load_sem,
    w_send,
    w_recv,
    t_send,
    t_recv,
    s_send,
    s_recv,
):
    layers, width = taps_ref.shape[0], taps_ref.shape[1]
    rows, feats = hidden_ref.shape
    piece = value_ref.shape[2]
    blocks = n_sp // n_tp
    channels = blocks * piece
    reach = width - 1
    nz = n_sp // 2
    s = lax.axis_index("sp")
    t = lax.axis_index("tp")
    z, y = s // 2, s % 2
    chip, core = t // 2, t % 2
    core_mate = chip * 2 + (1 - core)
    chip_mate = (1 - chip) * 2 + core
    far_mate = (1 - chip) * 2 + (1 - core)

    loads = []
    for level in range(layers):
        for kind, (source, target) in enumerate(
            (
                (value_ref.at[level], w_in.at[level, s, :, pl.ds(0, piece)]),
                (gate_ref.at[level], w_in.at[level, s, :, pl.ds(piece, piece)]),
                (
                    out_proj_ref.at[level],
                    w_out.at[level, pl.ds(pl.multiple_of(s * piece, piece), piece), :],
                ),
            )
        ):
            copy = pltpu.make_async_copy(source, target, load_sem.at[level, kind])
            copy.start()
            loads.append(copy)

    barrier = pltpu.get_barrier_semaphore()

    def greet(sp_index, tp_index):
        pl.semaphore_signal(barrier, inc=1, device_id=(sp_index, tp_index), device_id_type=MESH)

    up, down = z < nz - 1, z > 0
    corner_up = jnp.logical_and(up, y == 1)
    corner_down = jnp.logical_and(down, y == 0)
    for mate in (core_mate, chip_mate, far_mate):
        greet(s, mate)
    greet(z * 2 + 1 - y, t)
    for condition, target in (
        (up, s + 2),
        (down, s - 2),
        (corner_up, s + 1),
        (corner_down, s - 1),
    ):

        @pl.when(condition)
        def _(target=target):
            greet(target, t)

    mates = 4
    for condition in (up, down, corner_up, corner_down):
        mates = mates + condition.astype(jnp.int32)
    pl.semaphore_wait(barrier, mates)

    for copy in loads:
        copy.wait()

    half = feats // 2
    phases = []
    for level in range(layers):
        phases += [("in", level, 0), ("in", level, 1), ("out", level, 0)]

    def chunk(phase, owner, lot):
        kind, level, part_index = phases[phase]
        deep = half if kind == "in" else piece
        cut = deep - deep * SPLIT // 16 // 16 * 16
        low, size = (0, cut) if lot == 0 else (cut, deep - cut)
        if kind == "in":
            return w_in.at[level, owner, pl.ds(part_index * half + low, size), :]
        return w_out.at[level, pl.ds(pl.multiple_of(owner * piece, piece) + low, size), :]

    def weight_copy(phase, owner, way, lot):
        target = (s + 2, s - 2, z * 2 + 1 - y)[way]
        return pltpu.make_async_remote_copy(
            src_ref=chunk(phase, owner, lot),
            dst_ref=chunk(phase, owner, lot),
            send_sem=w_send.at[phase, lot, way, owner],
            recv_sem=w_recv.at[phase, lot, owner],
            device_id=(target, t),
            device_id_type=MESH,
        )

    def both_ways(phase, owner, lot):
        @pl.when(up)
        def _():
            weight_copy(phase, owner, 0, lot).start()

        @pl.when(down)
        def _():
            weight_copy(phase, owner, 1, lot).start()

    def own(phase):
        for lot in (1, 0):
            weight_copy(phase, s, 2, lot).start()
            both_ways(phase, s, lot)

    def hops(phase):
        across = z * 2 + 1 - y
        weight_copy(phase, across, 2, 1).wait_recv()
        both_ways(phase, across, 1)
        moves = ((y, 1), (y, 0), (1 - y, 1))
        for hop in range(1, nz):
            for column, lot in moves:

                @pl.when(z >= hop)
                def _(hop=hop, column=column, lot=lot):
                    owner = (z - hop) * 2 + column
                    weight_copy(phase, owner, 0, lot).wait_recv()

                    @pl.when(up)
                    def _():
                        weight_copy(phase, owner, 0, lot).start()

                    if lot == 0:
                        weight_copy(phase, owner, 2, lot).start()

                @pl.when(z + hop < nz)
                def _(hop=hop, column=column, lot=lot):
                    owner = (z + hop) * 2 + column
                    weight_copy(phase, owner, 1, lot).wait_recv()

                    @pl.when(down)
                    def _():
                        weight_copy(phase, owner, 1, lot).start()

                    if lot == 0:
                        weight_copy(phase, owner, 2, lot).start()

    def crossed(phase):
        for z_from in range(nz):
            weight_copy(phase, z_from * 2 + 1 - y, 2, 0).wait_recv()

    def sent(phase):
        for z_from in range(nz):
            for column, lot in ((y, 0), (y, 1), (1 - y, 1)):
                owner = z_from * 2 + column

                @pl.when(jnp.logical_and(z >= z_from, up))
                def _(owner=owner, lot=lot):
                    weight_copy(phase, owner, 0, lot).wait_send()

                @pl.when(jnp.logical_and(z <= z_from, down))
                def _(owner=owner, lot=lot):
                    weight_copy(phase, owner, 1, lot).wait_send()

            weight_copy(phase, z_from * 2 + y, 2, 0).wait_send()
        weight_copy(phase, s, 2, 1).wait_send()

    def tp_copy(level, slot, source, target, mate, sp_index=None):
        return pltpu.make_async_remote_copy(
            src_ref=source,
            dst_ref=target,
            send_sem=t_send.at[level, slot],
            recv_sem=t_recv.at[level, slot],
            device_id=(s if sp_index is None else sp_index, mate),
            device_id_type=MESH,
        )

    def prepare(level):
        gain = norm_ref[pl.ds(level, 1), :].astype(jnp.float32)
        ones = jnp.ones((8, feats), jnp.bfloat16)
        numbers = (((1,), (1,)), ((), ()))
        source = hidden_ref if level == 0 else out_ref
        for tile in range(rows // ROW_TILE):
            span = pl.ds(tile * ROW_TILE, ROW_TILE)
            wide = source[span, :].astype(jnp.float32)
            scaled[span, :] = (wide * gain).astype(jnp.bfloat16)
            square = wide * wide
            high = square.astype(jnp.bfloat16)
            low = (square - high.astype(jnp.float32)).astype(jnp.bfloat16)
            total = lax.dot_general(ones, high, numbers, preferred_element_type=jnp.float32)
            total = total + lax.dot_general(ones, low, numbers, preferred_element_type=jnp.float32)
            squares[level, t, :, span] = total
        for slot, mate in enumerate((core_mate, chip_mate, far_mate)):
            square_copy(level, slot, mate).start()

    def square_copy(level, slot, mate):
        return pltpu.make_async_remote_copy(
            src_ref=squares.at[level, t],
            dst_ref=squares.at[level, t],
            send_sem=s_send.at[level, slot],
            recv_sem=s_recv.at[level, slot],
            device_id=(s, mate),
            device_id_type=MESH,
        )

    def row_scales(level):
        for slot, mate in enumerate((core_mate, chip_mate, far_mate)):
            copy = square_copy(level, slot, mate)
            copy.wait_send()
            copy.wait_recv()
        total = squares[level, 0]
        for index in range(1, n_tp):
            total = total + squares[level, index]
        scale = lax.rsqrt(total / D + row_floor)
        return scale.T[:, 0:1]

    def products(level, owner):
        @pl.loop(0, blocks * (rows // ROW_TILE))
        def _(step):
            block = step // (rows // ROW_TILE)
            tile = step % (rows // ROW_TILE)
            span = pl.ds(pl.multiple_of(tile * ROW_TILE, ROW_TILE), ROW_TILE)
            part[owner, block, span, :] = jnp.dot(
                scaled[span, :],
                w_in[level, owner * blocks + block],
                preferred_element_type=jnp.float32,
            ).astype(jnp.bfloat16)

    base = 2 + blocks

    def core_copy(level, slot):
        owner = (far_mate, core_mate)[slot]
        return tp_copy(level, slot, part.at[owner], from_core.at[level, slot], core_mate)

    def chip_copy(level, block):
        return tp_copy(
            level, 2 + block, to_chip.at[block], from_chip.at[level, block], chip_mate
        )

    def halo_copy(level):
        return tp_copy(level, base + 3, halo_send, halo_recv.at[level], t, s + 1)

    def mixed_copy(level, slot):
        owner = (t, t, chip_mate)[slot]
        mate = (core_mate, chip_mate, core_mate)[slot]
        return tp_copy(
            level, base + slot, mixed.at[level, owner], mixed.at[level, owner], mate
        )

    def first_half(level):
        products(level, far_mate)
        core_copy(level, 0).start()
        products(level, chip_mate)
        core_copy(level, 0).wait_recv()
        for block in range(blocks):
            to_chip[block] = (
                part[chip_mate, block].astype(jnp.float32)
                + from_core[level, 0, block].astype(jnp.float32)
            ).astype(jnp.bfloat16)
            chip_copy(level, block).start()
        products(level, core_mate)
        core_copy(level, 1).start()
        products(level, t)
        core_copy(level, 1).wait_recv()

    def gating(level):
        scale = row_scales(level)
        for block in range(blocks):
            lanes = pl.ds(block * piece, piece)
            chip_copy(level, block).wait_recv()
            total = (
                part[t, block].astype(jnp.float32)
                + from_core[level, 1, block].astype(jnp.float32)
                + from_chip[level, block].astype(jnp.float32)
            ) * scale
            gated = (total[:, :piece] * jax.nn.sigmoid(total[:, piece:])).astype(jnp.bfloat16)
            halo_send[:, lanes] = gated[rows - HALO :]
            extended[pl.ds(HALO, rows), lanes] = gated.astype(jnp.float32)

        @pl.when(s < n_sp - 1)
        def _():
            halo_copy(level).start()

    def filtering(level):
        taps = taps_ref[level].astype(jnp.float32)
        bias = bias_ref[pl.ds(level, 1), :].astype(jnp.float32)
        ggain = ggain_ref[pl.ds(level, 1), :].astype(jnp.float32)
        gshift = gshift_ref[pl.ds(level, 1), :].astype(jnp.float32)

        @pl.when(s > 0)
        def _():
            halo_copy(level).wait_recv()
            extended[pl.ds(0, HALO), :] = halo_recv[level].astype(jnp.float32)

        @pl.when(s == 0)
        def _():
            extended[pl.ds(0, HALO), :] = jnp.zeros((HALO, channels), jnp.float32)

        @pl.loop(0, rows // CONV_TILE)
        def _(tile):
            start = pl.multiple_of(tile * CONV_TILE, CONV_TILE)
            window = extended[pl.ds(start, CONV_TILE + HALO), :]
            filtered = jnp.zeros((CONV_TILE, channels), jnp.float32) + bias
            for offset in range(width):
                low = HALO - reach + offset
                filtered = filtered + taps[offset : offset + 1, :] * window[low : low + CONV_TILE]
            mean = jnp.mean(filtered, axis=1, keepdims=True)
            centered = filtered - mean
            var = jnp.mean(centered * centered, axis=1, keepdims=True)
            normed = centered * lax.rsqrt(var + group_floor) * ggain + gshift
            mixed[level, t, pl.ds(start, CONV_TILE), :] = (
                normed * jax.nn.sigmoid(normed)
            ).astype(jnp.bfloat16)

        mixed_copy(level, 1).start()
        mixed_copy(level, 0).start()

    def relay(level):
        mixed_copy(level, 1).wait_recv()
        mixed_copy(level, 2).start()

    def projecting(level):
        mixed_copy(level, 0).wait_recv()
        mixed_copy(level, 2).wait_recv()
        source = hidden_ref if level == 0 else out_ref
        tiles = rows // ROW_TILE

        @pl.loop(0, tiles)
        def _(tile):
            span = pl.ds(pl.multiple_of(tile * ROW_TILE, ROW_TILE), ROW_TILE)
            total = source[span, :].astype(jnp.float32)
            for owner in range(n_tp):
                total = total + jnp.dot(
                    mixed[level, owner, span, :],
                    w_out[level, pl.ds(owner * channels, channels), :],
                    preferred_element_type=jnp.float32,
                )
            out_ref[span, :] = total.astype(jnp.bfloat16)

    def settle(level):
        for slot in range(2):
            core_copy(level, slot).wait_send()
        for block in range(blocks):
            chip_copy(level, block).wait_send()
        for slot in range(3):
            mixed_copy(level, slot).wait_send()

        @pl.when(s < n_sp - 1)
        def _():
            halo_copy(level).wait_send()

    own(0)
    own(1)
    prepare(0)
    for level in range(layers):
        first = 3 * level
        last = level == layers - 1
        if level == 0:
            hops(0)
            own(2)
            hops(1)
            if not last:
                own(3)
        crossed(first)
        crossed(first + 1)
        first_half(level)
        hops(first + 2)
        gating(level)
        if not last:
            hops(first + 3)
            own(first + 4)
        filtering(level)
        if not last:
            hops(first + 4)
            own(first + 5)
        relay(level)
        crossed(first + 2)
        projecting(level)
        settle(level)
        if not last:
            prepare(level + 1)
    for phase in range(len(phases)):
        sent(phase)


def fused(n_sp, n_tp, *arrays):
    hidden_in, norm_gain, value_proj = arrays[:3]
    rows, feats = hidden_in.shape
    layers = norm_gain.shape[0]
    piece = value_proj.shape[2]
    blocks = n_sp // n_tp
    channels = blocks * piece
    kinds = 3
    vmem = pl.BlockSpec(memory_space=pltpu.VMEM)
    hbm = pl.BlockSpec(memory_space=pl.ANY)
    low, wide = jnp.bfloat16, jnp.float32
    slots = 2 + blocks + 4
    return pl.pallas_call(
        lambda *refs: fused_kernel(n_sp, n_tp, *refs),
        out_shape=jax.ShapeDtypeStruct((rows, feats), low),
        in_specs=[vmem, vmem, hbm, hbm, vmem, vmem, vmem, vmem, hbm],
        out_specs=vmem,
        scratch_shapes=[
            pltpu.VMEM((layers, n_sp, feats, 2 * piece), low),
            pltpu.VMEM((layers, n_sp * piece, feats), low),
            pltpu.VMEM((rows, feats), low),
            pltpu.VMEM((n_tp, blocks, rows, 2 * piece), low),
            pltpu.VMEM((layers, 2, blocks, rows, 2 * piece), low),
            pltpu.VMEM((blocks, rows, 2 * piece), low),
            pltpu.VMEM((layers, blocks, rows, 2 * piece), low),
            pltpu.VMEM((HALO + rows, channels), wide),
            pltpu.VMEM((HALO, channels), low),
            pltpu.VMEM((layers, HALO, channels), low),
            pltpu.VMEM((layers, n_tp, rows, channels), low),
            pltpu.VMEM((layers, n_tp, 8, rows), wide),
            pltpu.SemaphoreType.DMA((layers, kinds)),
            pltpu.SemaphoreType.DMA((layers * kinds, 2, 3, n_sp)),
            pltpu.SemaphoreType.DMA((layers * kinds, 2, n_sp)),
            pltpu.SemaphoreType.DMA((layers, slots)),
            pltpu.SemaphoreType.DMA((layers, slots)),
            pltpu.SemaphoreType.DMA((layers, 3)),
            pltpu.SemaphoreType.DMA((layers, 3)),
        ],
        compiler_params=pltpu.CompilerParams(
            collective_id=0, has_side_effects=True, vmem_limit_bytes=VMEM_BYTES
        ),
    )(*arrays)


def solution(mesh):
    n_sp, n_tp = mesh.shape["sp"], mesh.shape["tp"]
    piece = C // n_sp
    small = n_tp == 4 and GROUPS == n_tp and n_sp % n_tp == 0 and piece % 128 == 0

    def local(*arrays):
        if small and arrays[0].shape[0] % ROW_TILE == 0:
            return fused(n_sp, n_tp, *arrays)
        return on_device(*arrays)

    return jax.shard_map(
        local,
        mesh=mesh,
        in_specs=(
            P("sp", "tp"),
            P(None, "tp"),
            P(None, "tp", "sp"),
            P(None, "tp", "sp"),
            P(None, None, "tp"),
            P(None, "tp"),
            P(None, "tp"),
            P(None, "tp"),
            P(None, "sp", "tp"),
        ),
        out_specs=P("sp", "tp"),
        check_vma=False,
    )
```

```python
import jax
import jax.numpy as jnp
from jax import lax
from jax.experimental import pallas as pl
from jax.experimental.pallas import tpu as pltpu
from jax.sharding import PartitionSpec as P

D = 4096
C = 1024
GROUPS = 4
WIDTH = 31


row_floor = 1e-06
group_floor = 1e-05


def passed_along(value, axis, steps):
    count = lax.axis_size(axis)
    initial, last = (max(0, -steps), min(count, count - steps))
    return lax.ppermute(value, axis, [(source, source + steps) for source in range(initial, last)])


def rms_normed(residual_rows, gain_part):
    wide_rows = residual_rows.astype(jnp.float32)
    squares = lax.psum(jnp.sum(wide_rows * wide_rows, axis=1), "tp")
    scale_rows = lax.rsqrt(squares / D + row_floor)
    return (wide_rows * scale_rows[:, None] * gain_part.astype(jnp.float32)[None, :]).astype(
        jnp.bfloat16
    )


def gated_input(normed_rows, w_value, w_gate):
    numbers = (((0,), (1,)), ((), ()))
    value_part = lax.dot_general(w_value, normed_rows, numbers, preferred_element_type=jnp.float32)
    gate_part = lax.dot_general(w_gate, normed_rows, numbers, preferred_element_type=jnp.float32)
    summed = lax.psum_scatter(
        jnp.stack([value_part, gate_part], axis=1).astype(jnp.bfloat16),
        "tp",
        scatter_dimension=0,
        tiled=True,
    ).astype(jnp.float32)
    return (summed[:, 0] * jax.nn.sigmoid(summed[:, 1])).astype(jnp.bfloat16)


def depthwise(extended, taps_part, bias_part, out_len):
    widened = extended.astype(jnp.float32)
    taps = taps_part.astype(jnp.float32)
    filtered = (
        jnp.zeros((extended.shape[0], out_len), jnp.float32)
        + bias_part.astype(jnp.float32)[:, None]
    )
    for offset in range(WIDTH):
        filtered = filtered + taps[offset][:, None] * widened[:, offset : offset + out_len]
    return filtered


def group_normed(filtered, gain_part, shift_part, group_size):
    channels, out_len = filtered.shape
    grouped = filtered.reshape(channels // group_size, group_size, out_len)
    group_mean = jnp.mean(grouped, axis=1, keepdims=True)
    centered = grouped - group_mean
    group_var = jnp.mean(centered * centered, axis=1, keepdims=True)
    scaled = (centered * lax.rsqrt(group_var + group_floor)).reshape(channels, out_len)
    scaled = (
        scaled * gain_part.astype(jnp.float32)[:, None] + shift_part.astype(jnp.float32)[:, None]
    )
    return jax.nn.silu(scaled).astype(jnp.bfloat16)


def project_out(mixed, w_out):
    return lax.dot_general(
        lax.all_gather(mixed, "tp", axis=0, tiled=True),
        w_out,
        (((0,), (0,)), ((), ())),
        preferred_element_type=jnp.float32,
    )


def on_device(
    hidden_in,
    norm_gain,
    value_proj,
    gate_proj,
    conv_taps,
    conv_bias,
    group_gain,
    group_shift,
    out_proj,
):
    tok_rows = hidden_in.shape[0]
    layers = norm_gain.shape[0]
    reach_back = WIDTH - 1
    group_size = C // GROUPS
    all_value, all_gate, all_out = (
        lax.all_gather(value_proj, "sp", axis=2, tiled=True),
        lax.all_gather(gate_proj, "sp", axis=2, tiled=True),
        lax.all_gather(out_proj, "sp", axis=1, tiled=True),
    )
    residual_rows = hidden_in
    for level in range(layers):
        w_value, w_gate, w_out = (all_value[level], all_gate[level], all_out[level])
        normed_rows = rms_normed(residual_rows, norm_gain[level])
        gated = gated_input(normed_rows, w_value, w_gate)
        before = passed_along(gated[:, tok_rows - reach_back :], "sp", 1)
        extended = jnp.concatenate([before, gated], axis=1)
        out_len = extended.shape[1] - reach_back
        filtered = depthwise(extended, conv_taps[level], conv_bias[level], out_len)
        mixed = group_normed(filtered, group_gain[level], group_shift[level], group_size)
        update = project_out(mixed, w_out)
        kept_rows = residual_rows
        residual_rows = (kept_rows.astype(jnp.float32) + update).astype(jnp.bfloat16)
    return residual_rows


MESH = pl.DeviceIdType.MESH
HALO = 32
ROW_TILE = 256
CONV_TILE = 64
VMEM_BYTES = 62 * 1024 * 1024
SPLIT = 3


def fused_kernel(
    n_sp,
    n_tp,
    hidden_ref,
    norm_ref,
    value_ref,
    gate_ref,
    taps_ref,
    bias_ref,
    ggain_ref,
    gshift_ref,
    out_proj_ref,
    out_ref,
    w_in,
    w_out,
    scaled,
    part,
    from_core,
    to_chip,
    from_chip,
    extended,
    halo_send,
    halo_recv,
    mixed,
    squares,
    load_sem,
    w_send,
    w_recv,
    t_send,
    t_recv,
    s_send,
    s_recv,
):
    layers, width = taps_ref.shape[0], taps_ref.shape[1]
    rows, feats = hidden_ref.shape
    piece = value_ref.shape[2]
    blocks = n_sp // n_tp
    channels = blocks * piece
    reach = width - 1
    nz = n_sp // 2
    s = lax.axis_index("sp")
    t = lax.axis_index("tp")
    z, y = s // 2, s % 2
    chip, core = t // 2, t % 2
    core_mate = chip * 2 + (1 - core)
    chip_mate = (1 - chip) * 2 + core
    far_mate = (1 - chip) * 2 + (1 - core)

    loads = []
    for level in range(layers):
        for kind, (source, target) in enumerate(
            (
                (value_ref.at[level], w_in.at[level, s, :, pl.ds(0, piece)]),
                (gate_ref.at[level], w_in.at[level, s, :, pl.ds(piece, piece)]),
                (
                    out_proj_ref.at[level],
                    w_out.at[level, pl.ds(pl.multiple_of(s * piece, piece), piece), :],
                ),
            )
        ):
            copy = pltpu.make_async_copy(source, target, load_sem.at[level, kind])
            copy.start()
            loads.append(copy)

    barrier = pltpu.get_barrier_semaphore()

    def greet(sp_index, tp_index):
        pl.semaphore_signal(barrier, inc=1, device_id=(sp_index, tp_index), device_id_type=MESH)

    up, down = z < nz - 1, z > 0
    corner_up = jnp.logical_and(up, y == 1)
    corner_down = jnp.logical_and(down, y == 0)
    for mate in (core_mate, chip_mate, far_mate):
        greet(s, mate)
    greet(z * 2 + 1 - y, t)
    for condition, target in (
        (up, s + 2),
        (down, s - 2),
        (corner_up, s + 1),
        (corner_down, s - 1),
    ):

        @pl.when(condition)
        def _(target=target):
            greet(target, t)

    mates = 4
    for condition in (up, down, corner_up, corner_down):
        mates = mates + condition.astype(jnp.int32)
    pl.semaphore_wait(barrier, mates)

    for copy in loads:
        copy.wait()

    half = feats // 2
    phases = []
    for level in range(layers):
        phases += [("in", level, 0), ("in", level, 1), ("out", level, 0)]

    def chunk(phase, owner, lot):
        kind, level, part_index = phases[phase]
        deep = half if kind == "in" else piece
        cut = deep - deep * SPLIT // 16 // 16 * 16
        low, size = (0, cut) if lot == 0 else (cut, deep - cut)
        if kind == "in":
            return w_in.at[level, owner, pl.ds(part_index * half + low, size), :]
        return w_out.at[level, pl.ds(pl.multiple_of(owner * piece, piece) + low, size), :]

    def weight_copy(phase, owner, way, lot):
        target = (s + 2, s - 2, z * 2 + 1 - y)[way]
        return pltpu.make_async_remote_copy(
            src_ref=chunk(phase, owner, lot),
            dst_ref=chunk(phase, owner, lot),
            send_sem=w_send.at[phase, lot, way, owner],
            recv_sem=w_recv.at[phase, lot, owner],
            device_id=(target, t),
            device_id_type=MESH,
        )

    def both_ways(phase, owner, lot):
        @pl.when(up)
        def _():
            weight_copy(phase, owner, 0, lot).start()

        @pl.when(down)
        def _():
            weight_copy(phase, owner, 1, lot).start()

    def own(phase):
        for lot in (1, 0):
            weight_copy(phase, s, 2, lot).start()
            both_ways(phase, s, lot)

    def hops(phase):
        across = z * 2 + 1 - y
        weight_copy(phase, across, 2, 1).wait_recv()
        both_ways(phase, across, 1)
        moves = ((y, 1), (y, 0), (1 - y, 1))
        for hop in range(1, nz):
            for column, lot in moves:

                @pl.when(z >= hop)
                def _(hop=hop, column=column, lot=lot):
                    owner = (z - hop) * 2 + column
                    weight_copy(phase, owner, 0, lot).wait_recv()

                    @pl.when(up)
                    def _():
                        weight_copy(phase, owner, 0, lot).start()

                    if lot == 0:
                        weight_copy(phase, owner, 2, lot).start()

                @pl.when(z + hop < nz)
                def _(hop=hop, column=column, lot=lot):
                    owner = (z + hop) * 2 + column
                    weight_copy(phase, owner, 1, lot).wait_recv()

                    @pl.when(down)
                    def _():
                        weight_copy(phase, owner, 1, lot).start()

                    if lot == 0:
                        weight_copy(phase, owner, 2, lot).start()

    def crossed(phase):
        for z_from in range(nz):
            weight_copy(phase, z_from * 2 + 1 - y, 2, 0).wait_recv()

    def sent(phase):
        for z_from in range(nz):
            for column, lot in ((y, 0), (y, 1), (1 - y, 1)):
                owner = z_from * 2 + column

                @pl.when(jnp.logical_and(z >= z_from, up))
                def _(owner=owner, lot=lot):
                    weight_copy(phase, owner, 0, lot).wait_send()

                @pl.when(jnp.logical_and(z <= z_from, down))
                def _(owner=owner, lot=lot):
                    weight_copy(phase, owner, 1, lot).wait_send()

            weight_copy(phase, z_from * 2 + y, 2, 0).wait_send()
        weight_copy(phase, s, 2, 1).wait_send()

    def tp_copy(level, slot, source, target, mate, sp_index=None):
        return pltpu.make_async_remote_copy(
            src_ref=source,
            dst_ref=target,
            send_sem=t_send.at[level, slot],
            recv_sem=t_recv.at[level, slot],
            device_id=(s if sp_index is None else sp_index, mate),
            device_id_type=MESH,
        )

    def prepare(level):
        gain = norm_ref[pl.ds(level, 1), :].astype(jnp.float32)
        ones = jnp.ones((8, feats), jnp.bfloat16)
        numbers = (((1,), (1,)), ((), ()))
        source = hidden_ref if level == 0 else out_ref
        for tile in range(rows // ROW_TILE):
            span = pl.ds(tile * ROW_TILE, ROW_TILE)
            wide = source[span, :].astype(jnp.float32)
            scaled[span, :] = (wide * gain).astype(jnp.bfloat16)
            square = wide * wide
            high = square.astype(jnp.bfloat16)
            low = (square - high.astype(jnp.float32)).astype(jnp.bfloat16)
            total = lax.dot_general(ones, high, numbers, preferred_element_type=jnp.float32)
            total = total + lax.dot_general(ones, low, numbers, preferred_element_type=jnp.float32)
            squares[level, t, :, span] = total
        for slot, mate in enumerate((core_mate, chip_mate, far_mate)):
            square_copy(level, slot, mate).start()

    def square_copy(level, slot, mate):
        return pltpu.make_async_remote_copy(
            src_ref=squares.at[level, t],
            dst_ref=squares.at[level, t],
            send_sem=s_send.at[level, slot],
            recv_sem=s_recv.at[level, slot],
            device_id=(s, mate),
            device_id_type=MESH,
        )

    def row_scales(level):
        for slot, mate in enumerate((core_mate, chip_mate, far_mate)):
            copy = square_copy(level, slot, mate)
            copy.wait_send()
            copy.wait_recv()
        total = squares[level, 0]
        for index in range(1, n_tp):
            total = total + squares[level, index]
        scale = lax.rsqrt(total / D + row_floor)
        return scale.T[:, 0:1]

    def products(level, owner):
        @pl.loop(0, blocks * (rows // ROW_TILE))
        def _(step):
            block = step // (rows // ROW_TILE)
            tile = step % (rows // ROW_TILE)
            span = pl.ds(pl.multiple_of(tile * ROW_TILE, ROW_TILE), ROW_TILE)
            part[owner, block, span, :] = jnp.dot(
                scaled[span, :],
                w_in[level, owner * blocks + block],
                preferred_element_type=jnp.float32,
            ).astype(jnp.bfloat16)

    base = 2 + blocks
    parts = rows // ROW_TILE
    order = tuple(reversed(range(parts)))

    def core_copy(level, slot):
        owner = (far_mate, core_mate)[slot]
        return tp_copy(level, slot, part.at[owner], from_core.at[level, slot], core_mate)

    def chip_copy(level, block):
        return tp_copy(
            level, 2 + block, to_chip.at[block], from_chip.at[level, block], chip_mate
        )

    def halo_copy(level):
        return tp_copy(level, base + 3 * parts, halo_send, halo_recv.at[level], t, s + 1)

    def mixed_copy(level, slot, third):
        owner = (t, t, chip_mate)[slot]
        mate = (core_mate, chip_mate, core_mate)[slot]
        block = mixed.at[level, owner, pl.ds(third * ROW_TILE, ROW_TILE), :]
        return tp_copy(level, base + slot * parts + third, block, block, mate)

    def first_half(level):
        products(level, far_mate)
        core_copy(level, 0).start()
        products(level, chip_mate)
        core_copy(level, 0).wait_recv()
        for block in range(blocks):
            to_chip[block] = (
                part[chip_mate, block].astype(jnp.float32)
                + from_core[level, 0, block].astype(jnp.float32)
            ).astype(jnp.bfloat16)
            chip_copy(level, block).start()
        products(level, core_mate)
        core_copy(level, 1).start()
        products(level, t)
        core_copy(level, 1).wait_recv()

    def gating(level):
        scale = row_scales(level)
        for block in range(blocks):
            lanes = pl.ds(block * piece, piece)
            chip_copy(level, block).wait_recv()
            total = (
                part[t, block].astype(jnp.float32)
                + from_core[level, 1, block].astype(jnp.float32)
                + from_chip[level, block].astype(jnp.float32)
            ) * scale
            gated = (total[:, :piece] * jax.nn.sigmoid(total[:, piece:])).astype(jnp.bfloat16)
            halo_send[:, lanes] = gated[rows - HALO :]
            extended[pl.ds(HALO, rows), lanes] = gated.astype(jnp.float32)

        @pl.when(s < n_sp - 1)
        def _():
            halo_copy(level).start()

    def filtering(level):
        taps = taps_ref[level].astype(jnp.float32)
        bias = bias_ref[pl.ds(level, 1), :].astype(jnp.float32)
        ggain = ggain_ref[pl.ds(level, 1), :].astype(jnp.float32)
        gshift = gshift_ref[pl.ds(level, 1), :].astype(jnp.float32)

        per_part = ROW_TILE // CONV_TILE
        for third in order:
            if third == 0:
                @pl.when(s > 0)
                def _():
                    halo_copy(level).wait_recv()
                    extended[pl.ds(0, HALO), :] = halo_recv[level].astype(jnp.float32)

                @pl.when(s == 0)
                def _():
                    extended[pl.ds(0, HALO), :] = jnp.zeros((HALO, channels), jnp.float32)

            @pl.loop(third * per_part, (third + 1) * per_part)
            def _(tile):
                start = pl.multiple_of(tile * CONV_TILE, CONV_TILE)
                window = extended[pl.ds(start, CONV_TILE + HALO), :]
                filtered = jnp.zeros((CONV_TILE, channels), jnp.float32) + bias
                for offset in range(width):
                    low = HALO - reach + offset
                    filtered = filtered + taps[offset : offset + 1, :] * window[low : low + CONV_TILE]
                mean = jnp.mean(filtered, axis=1, keepdims=True)
                centered = filtered - mean
                var = jnp.mean(centered * centered, axis=1, keepdims=True)
                normed = centered * lax.rsqrt(var + group_floor) * ggain + gshift
                mixed[level, t, pl.ds(start, CONV_TILE), :] = (
                    normed * jax.nn.sigmoid(normed)
                ).astype(jnp.bfloat16)

            mixed_copy(level, 1, third).start()
            mixed_copy(level, 0, third).start()

    def relay(level, third):
        mixed_copy(level, 1, third).wait_recv()
        mixed_copy(level, 2, third).start()

    def projecting(level, third):
        mixed_copy(level, 0, third).wait_recv()
        mixed_copy(level, 2, third).wait_recv()
        source = hidden_ref if level == 0 else out_ref
        span = pl.ds(third * ROW_TILE, ROW_TILE)
        total = source[span, :].astype(jnp.float32)
        for owner in range(n_tp):
            total = total + jnp.dot(
                mixed[level, owner, span, :],
                w_out[level, pl.ds(owner * channels, channels), :],
                preferred_element_type=jnp.float32,
            )
        out_ref[span, :] = total.astype(jnp.bfloat16)

    def settle(level):
        for slot in range(2):
            core_copy(level, slot).wait_send()
        for block in range(blocks):
            chip_copy(level, block).wait_send()
        for slot in range(3):
            for third in order:
                mixed_copy(level, slot, third).wait_send()

        @pl.when(s < n_sp - 1)
        def _():
            halo_copy(level).wait_send()

    own(0)
    own(1)
    prepare(0)
    for level in range(layers):
        first = 3 * level
        last = level == layers - 1
        if level == 0:
            hops(0)
            own(2)
            hops(1)
            if not last:
                own(3)
        crossed(first)
        crossed(first + 1)
        first_half(level)
        hops(first + 2)
        gating(level)
        if not last:
            hops(first + 3)
            own(first + 4)
        filtering(level)
        if not last:
            hops(first + 4)
            own(first + 5)
        relay(level, order[0])
        crossed(first + 2)
        for index in range(1, parts):
            relay(level, order[index])
            projecting(level, order[index - 1])
        projecting(level, order[-1])
        settle(level)
        if not last:
            prepare(level + 1)
    for phase in range(len(phases)):
        sent(phase)


def fused(n_sp, n_tp, *arrays):
    hidden_in, norm_gain, value_proj = arrays[:3]
    rows, feats = hidden_in.shape
    layers = norm_gain.shape[0]
    piece = value_proj.shape[2]
    blocks = n_sp // n_tp
    channels = blocks * piece
    kinds = 3
    vmem = pl.BlockSpec(memory_space=pltpu.VMEM)
    hbm = pl.BlockSpec(memory_space=pl.ANY)
    low, wide = jnp.bfloat16, jnp.float32
    slots = 2 + blocks + 3 * (rows // ROW_TILE) + 1
    return pl.pallas_call(
        lambda *refs: fused_kernel(n_sp, n_tp, *refs),
        out_shape=jax.ShapeDtypeStruct((rows, feats), low),
        in_specs=[vmem, vmem, hbm, hbm, vmem, vmem, vmem, vmem, hbm],
        out_specs=vmem,
        scratch_shapes=[
            pltpu.VMEM((layers, n_sp, feats, 2 * piece), low),
            pltpu.VMEM((layers, n_sp * piece, feats), low),
            pltpu.VMEM((rows, feats), low),
            pltpu.VMEM((n_tp, blocks, rows, 2 * piece), low),
            pltpu.VMEM((layers, 2, blocks, rows, 2 * piece), low),
            pltpu.VMEM((blocks, rows, 2 * piece), low),
            pltpu.VMEM((layers, blocks, rows, 2 * piece), low),
            pltpu.VMEM((HALO + rows, channels), wide),
            pltpu.VMEM((HALO, channels), low),
            pltpu.VMEM((layers, HALO, channels), low),
            pltpu.VMEM((layers, n_tp, rows, channels), low),
            pltpu.VMEM((layers, n_tp, 8, rows), wide),
            pltpu.SemaphoreType.DMA((layers, kinds)),
            pltpu.SemaphoreType.DMA((layers * kinds, 2, 3, n_sp)),
            pltpu.SemaphoreType.DMA((layers * kinds, 2, n_sp)),
            pltpu.SemaphoreType.DMA((layers, slots)),
            pltpu.SemaphoreType.DMA((layers, slots)),
            pltpu.SemaphoreType.DMA((layers, 3)),
            pltpu.SemaphoreType.DMA((layers, 3)),
        ],
        compiler_params=pltpu.CompilerParams(
            collective_id=0, has_side_effects=True, vmem_limit_bytes=VMEM_BYTES
        ),
    )(*arrays)


def solution(mesh):
    n_sp, n_tp = mesh.shape["sp"], mesh.shape["tp"]
    piece = C // n_sp
    small = n_tp == 4 and GROUPS == n_tp and n_sp % n_tp == 0 and piece % 128 == 0

    def local(*arrays):
        if small and arrays[0].shape[0] % ROW_TILE == 0:
            return fused(n_sp, n_tp, *arrays)
        return on_device(*arrays)

    return jax.shard_map(
        local,
        mesh=mesh,
        in_specs=(
            P("sp", "tp"),
            P(None, "tp"),
            P(None, "tp", "sp"),
            P(None, "tp", "sp"),
            P(None, None, "tp"),
            P(None, "tp"),
            P(None, "tp"),
            P(None, "tp"),
            P(None, "sp", "tp"),
        ),
        out_specs=P("sp", "tp"),
        check_vma=False,
    )
```
